32 devices in a mesh: grp: 2 (over y), fs: 4 (over z), tp: 4 (over x, core).
Axes of the slice: x: 2, y: 2, z: 4, core: 2. Of those that a mesh axis runs over, the one named last changes fastest.
Arguments:
- tokens: bfloat16 [1536, 2048], P(('grp', 'fs'), 'tp'), parts along dimension 0, may hold values from -40 to 40
- routes: int32 [1536, 2], P(('grp', 'fs')), parts along dimension 0, may hold values from 0 to 3, all different within a row; in each aligned block of 192 rows (0 to 191, 192 to 383, ...) at most 112 rows name the same one
- routing_weight: float32 [1536, 2], P(('grp', 'fs')), parts along dimension 0, may hold values from 0.1 to 0.6
- norm_gain_vector: float32 [2048], P('tp'), may hold values from 0.1 to 1.9
- expert_gate: float32 [4, 512, 2048], P(None, 'fs', 'tp'), may hold values from -0.125 to 0.125
- expert_up: float32 [4, 512, 2048], P(None, 'fs', 'tp'), may hold values from -0.125 to 0.125
- expert_down: float32 [4, 512, 2048], P(None, 'fs', 'tp'), may hold values from -0.25 to 0.25
- shared_gate: float32 [512, 2048], P('fs', 'tp'), may hold values from -0.125 to 0.125
- shared_up: float32 [512, 2048], P('fs', 'tp'), may hold values from -0.125 to 0.125
- shared_down: float32 [512, 2048], P('fs', 'tp'), may hold values from -0.25 to 0.25
Outputs:
- mixed: bfloat16 [1536, 2048], P(('grp', 'fs'), 'tp'), parts along dimension 0
- gate_served: bfloat16 [8, 512, 2048], P(('grp', 'fs'), None, 'tp'), parts along dimension 0
- up_served: bfloat16 [8, 512, 2048], P(('grp', 'fs'), None, 'tp'), parts along dimension 0
- down_served: bfloat16 [8, 512, 2048], P(('grp', 'fs'), None, 'tp'), parts along dimension 0
- shared_gate_served: bfloat16 [1024, 2048], P('grp', 'tp'), parts along dimension 0
- shared_up_served: bfloat16 [1024, 2048], P('grp', 'tp'), parts along dimension 0
- shared_down_served: bfloat16 [1024, 2048], P('grp', 'tp'), parts along dimension 0
The draws below stay inside these ranges and needn't reach their ends.
There are 2 independent parts, one for each index of `grp`. The reference program is written for one: setup_inputs(seed, part) draws one part's arguments, and reference() takes and returns one part's arrays. A program takes and returns all parts, laid end to end along the dimension named above; an argument that names none is the same for every part. Nothing has to cross between parts.
Inputs may be any that keep to these rules, and one draw needn't show every extreme that they name: `routes`: each row names 2 different experts. In each aligned block of 192 rows no expert is named by more than 112 rows, and in some block an expert is named by exactly 112 rows.
All inputs are finite; a program needn't handle non-finite values.
Results may differ from the reference program's by a relative error of at most 0.022.
Values may be sent and summed in bfloat16 or wider, within the bound.
A program may use at most 64 MiB of HBM per device.

```python
import math
import jax
import jax.numpy as jnp
import numpy as np
from jax import lax

D = 2048
FF = 512
SFF = 512
TOK_G = 192
EXPERTS = 4
TOPK = 2
CAP = 112
TOKENS = 768
N_FS = 4
N_TP = 4


def draw_tokens(key, part):
    base_key = jax.random.fold_in(key, 11)
    first, second = jax.random.split(base_key, 2)
    column = jnp.arange(D).astype(jnp.float32)
    trend = 1.0 + 2.0 * column / (D - 1)
    rough = jnp.exp(jax.random.uniform(second, (D,), jnp.float32) * jnp.log(10.0))
    scales = trend * rough
    scales = scales / jnp.sqrt(jnp.mean(scales * scales))
    values = jax.random.normal(first, (TOKENS, D), jnp.float32) * scales[None, :]
    return jnp.clip(values, -40.0, 40.0).astype(jnp.bfloat16)


def shard_levels(stream_key, extent, shards, smallest, top_value):
    def one(dim, parts):
        steps = jax.random.uniform(jax.random.fold_in(jax.random.fold_in(stream_key, 6), dim), (parts,), jnp.float32, smallest / len(shards), top_value / len(shards))
        return jnp.repeat(jnp.exp(steps), extent[dim] // parts).reshape((-1,) + (1,) * (len(extent) - dim - 1))

    factor_of = one(*shards[0])
    for cut in shards[1:]:
        factor_of = factor_of * one(*cut)
    return factor_of


def deal_out(key, own, number, rows, amount, top, most, slope):
    order = jax.random.permutation(key, amount)
    packed, usual = portions_of(amount, rows * top, most, slope, True), portions_of(amount, rows * top, most, slope, False)
    places = jnp.arange(amount)

    def named(sizes, rotation):
        used = int((sizes > 0).sum())
        fixed = max(1, used // 4)
        moved = fixed + (places - fixed + rotation * (used - fixed)) % max(1, amount - fixed)
        return jnp.zeros((amount,), jnp.int32).at[order[jnp.where(places < fixed, places, moved)]].set(jnp.asarray(sizes, jnp.int32))

    sizes = jnp.where(number % 4 == 0, named(packed, number // 4), named(usual, number - number // 4 - 1))
    mixed = jax.random.permutation(jax.random.fold_in(own, 3), amount)
    giver, taker = mixed[0:amount // 2 * 2:2], mixed[1:amount // 2 * 2:2]
    margin = jnp.minimum(sizes[giver] - 1, most - sizes[taker]) // 2
    margin = jnp.where((giver == order[0]) | (taker == order[0]) | (sizes[taker] == 0), 0, jnp.maximum(margin, 0))
    moved = jax.random.randint(jax.random.fold_in(own, 4), (amount // 2,), 0, 1 << 20) % (margin + 1)
    sizes = sizes.at[giver].add(-moved).at[taker].add(moved)
    labels = jnp.searchsorted(jnp.cumsum(sizes), jnp.arange(rows * top), side="right").astype(jnp.int32)
    grid = labels.reshape(top, rows).T
    grid = grid[jax.random.permutation(jax.random.fold_in(own, 1), rows)]
    rotation = jax.random.randint(jax.random.fold_in(own, 2), (rows, 1), 0, top)
    return jnp.take_along_axis(grid, (jnp.arange(top)[None, :] + rotation) % top, axis=1)


def portions_of(count, total, most, slope, full):
    weights = [(1 << 20) // math.isqrt(standing ** slope) + 1 for standing in range(1, count + 1)]
    largest = most if full else min(most, max(-(-total // count), total * weights[0] // sum(weights)))
    least = 1 if total - largest >= count - 1 else 0
    counts, spare = [largest] + [least] * (count - 1), total - largest - least * (count - 1)
    while spare > 0:
        candidates = [i for i in range(1, count) if counts[i] < largest] or [i for i in range(1, count) if counts[i] < most]
        mass, left = sum([weights[i] for i in candidates]), spare
        for i in candidates:
            extra = min(most - counts[i], max(1, left * weights[i] // mass), spare)
            counts[i] = counts[i] + extra
            spare = spare - extra
    return np.array(counts)


def noise(key, dims, spread, reach, cuts=(), held_as=jnp.bfloat16):
    drawn = jax.random.normal(key, dims, jnp.float32) * spread
    if len(cuts) > 0:
        drawn = shard_levels(key, dims, cuts, -0.22, 0.18) * drawn
    return jnp.clip(drawn, min=-reach, max=reach).astype(held_as)


def setup_inputs(seed: int = 0, part: int = 0) -> dict:
    splits = jax.random.split(jax.random.key(seed), 11)
    part_splits = jax.random.split(jax.random.fold_in(splits[10], part), 11)
    tokens = draw_tokens(jax.random.fold_in(jax.random.fold_in(splits[10], part), 71), part)
    routes_keys = jax.random.split(jax.random.fold_in(part_splits[1], 1), TOKENS // TOK_G)
    routes_turns = jax.random.permutation(jax.random.fold_in(part_splits[1], 3), TOKENS // TOK_G)
    routes = jax.vmap(lambda own, number: deal_out(jax.random.fold_in(part_splits[1], 2), own, number, TOK_G, EXPERTS, TOPK, CAP, 1))(routes_keys, routes_turns).reshape((TOKENS, TOPK))
    routing_weight = jnp.clip(0.1 + 0.5 * jax.random.uniform(part_splits[2], (TOKENS, TOPK), jnp.float32) ** shard_levels(part_splits[2], (TOKENS, TOPK), ((0, 4),), -0.2, 0.2), 0.1, 0.6)
    norm_gain_vector = jnp.clip(1.0 + 0.18 * jax.random.normal(splits[3], (D,), jnp.float32), 0.1, 1.9)
    expert_gate = noise(splits[4], (EXPERTS, FF, D), D ** -0.5, 0.125, ((1, 4), (2, 4)), jnp.float32)
    expert_up = noise(splits[5], (EXPERTS, FF, D), D ** -0.5, 0.125, ((1, 4), (2, 4)), jnp.float32)
    expert_down = noise(splits[6], (EXPERTS, FF, D), FF ** -0.5, 0.25, ((1, 4), (2, 4)), jnp.float32)
    shared_gate = noise(splits[7], (SFF, D), D ** -0.5, 0.125, ((0, 4), (1, 4)), jnp.float32)
    shared_up = noise(splits[8], (SFF, D), D ** -0.5, 0.125, ((0, 4), (1, 4)), jnp.float32)
    shared_down = noise(splits[9], (SFF, D), SFF ** -0.5, 0.25, ((0, 4), (1, 4)), jnp.float32)
    return {"tokens": tokens, "routes": routes, "routing_weight": routing_weight, "norm_gain_vector": norm_gain_vector, "expert_gate": expert_gate, "expert_up": expert_up, "expert_down": expert_down, "shared_gate": shared_gate, "shared_up": shared_up, "shared_down": shared_down}


norm_eps = 1e-06

def block_sums(rows, weight):
    count = rows.shape[0]
    outs = weight.shape[0]
    part = D // N_TP
    left_operand = rows.astype(jnp.float32).reshape(count, N_TP, part)
    right_operand = weight.astype(jnp.float32).reshape(outs, N_TP, part)
    fragments = jnp.einsum('ucb,xcb->cux', left_operand, right_operand)
    rounded = lax.optimization_barrier(fragments.astype(jnp.bfloat16))
    return lax.optimization_barrier(jnp.sum(rounded.astype(jnp.float32), axis=0))

def reference(tokens, routes, routing_weight, norm_gain_vector, expert_gate, expert_up, expert_down, shared_gate, shared_up, shared_down):
    gate_served = (expert_gate * norm_gain_vector[None, None, :]).astype(jnp.bfloat16)
    up_served = (expert_up * norm_gain_vector[None, None, :]).astype(jnp.bfloat16)
    down_served = expert_down.astype(jnp.bfloat16)
    shared_gate_served = (shared_gate * norm_gain_vector[None, :]).astype(jnp.bfloat16)
    shared_up_served = (shared_up * norm_gain_vector[None, :]).astype(jnp.bfloat16)
    shared_down_served = shared_down.astype(jnp.bfloat16)
    values = tokens.astype(jnp.float32)
    squares = lax.optimization_barrier(jnp.sum(values * values, axis=1, keepdims=True))
    normed = (values * lax.rsqrt(squares / D + norm_eps)).astype(jnp.bfloat16)
    grouped = routes.reshape(N_FS, TOK_G * TOPK)
    onehot = (grouped[:, :, None] == jnp.arange(EXPERTS, dtype=jnp.int32)[None, None, :]).astype(jnp.int32)
    earlier = jnp.cumsum(onehot, axis=1) - onehot
    slot_index = lax.optimization_barrier(jnp.sum(earlier * onehot, axis=2))
    blocks = jnp.arange(N_FS, dtype=jnp.int32)[:, None]
    target = (grouped * (N_FS * CAP) + blocks * CAP + slot_index).reshape(-1).astype(jnp.int32)
    token_ids = jnp.repeat(jnp.arange(TOKENS, dtype=jnp.int32), TOPK)
    row_table = jnp.full((EXPERTS * N_FS * CAP,), TOKENS, jnp.int32).at[target].set(token_ids)
    row_table = row_table.reshape(EXPERTS, N_FS * CAP)
    weight_table = jnp.zeros((EXPERTS * N_FS * CAP,), jnp.float32).at[target].set(routing_weight.reshape(-1).astype(jnp.float32))
    weight_table = weight_table.reshape(EXPERTS, N_FS * CAP)
    padded = jnp.concatenate([normed, jnp.zeros((1, D), jnp.bfloat16)], axis=0)

    def one_expert(total, items):
        row_ids, weights, gate_w, up_w, down_w = items
        rows = padded[row_ids]
        hidden = (jax.nn.silu(block_sums(rows, gate_w)) * block_sums(rows, up_w)).astype(jnp.bfloat16)
        produced = jnp.dot(hidden, down_w, preferred_element_type=jnp.float32).astype(jnp.bfloat16)
        return (total.at[row_ids].add(weights[:, None] * produced.astype(jnp.float32)), None)
    routed, _ = lax.scan(one_expert, jnp.zeros((TOKENS + 1, D), jnp.float32), (row_table, weight_table, gate_served, up_served, down_served))
    shared_hidden = (jax.nn.silu(block_sums(normed, shared_gate_served)) * block_sums(normed, shared_up_served)).astype(jnp.bfloat16)
    shared_out = jnp.dot(shared_hidden, shared_down_served, preferred_element_type=jnp.float32)
    mixed = (routed[:TOKENS] + shared_out).astype(jnp.bfloat16)
    return (mixed, gate_served, up_served, down_served, shared_gate_served, shared_up_served, shared_down_served)
```

```python
import functools

import jax
import jax.numpy as jnp
from jax import lax
from jax.experimental import pallas as pl
from jax.experimental.pallas import tpu as pltpu
from jax.sharding import PartitionSpec as P

norm_eps = 1e-06


def dense_rows(rows, weight):
    return lax.dot_general(
        rows, weight, (((1,), (1,)), ((), ())), preferred_element_type=jnp.float32
    )


def per_device_plain(
    tokens,
    routes,
    routing_weight,
    norm_gain_vector,
    expert_gate,
    expert_up,
    expert_down,
    shared_gate,
    shared_up,
    shared_down,
):
    tok_rows, portion_width = tokens.shape
    model_width = portion_width * lax.axis_size("tp")
    experts = expert_gate.shape[0]
    top_count = routes.shape[1]
    capacity = tok_rows * top_count * 7 // (6 * experts)
    gate_round = (expert_gate * norm_gain_vector[None, None, :]).astype(jnp.bfloat16)
    up_round = (expert_up * norm_gain_vector[None, None, :]).astype(jnp.bfloat16)
    down_round = expert_down.astype(jnp.bfloat16)
    gate_refreshed, up_new, down_new = (
        lax.all_to_all(gate_round, "fs", split_axis=0, concat_axis=1, tiled=True),
        lax.all_to_all(up_round, "fs", split_axis=0, concat_axis=1, tiled=True),
        lax.all_to_all(down_round, "fs", split_axis=0, concat_axis=1, tiled=True),
    )
    shared_g, shared_u, shared_d = (
        lax.all_gather(
            (shared_gate * norm_gain_vector[None, :]).astype(jnp.bfloat16), "fs", axis=0, tiled=True
        ),
        lax.all_gather(
            (shared_up * norm_gain_vector[None, :]).astype(jnp.bfloat16), "fs", axis=0, tiled=True
        ),
        lax.all_gather(shared_down.astype(jnp.bfloat16), "fs", axis=0, tiled=True),
    )
    values = tokens.astype(jnp.float32)
    totals = lax.psum(jnp.sum(values * values, axis=1), "tp")
    normed = (values * lax.rsqrt(totals / model_width + norm_eps)[:, None]).astype(jnp.bfloat16)
    flat_expert = routes.reshape(-1)
    onehot = (flat_expert[:, None] == jnp.arange(experts, dtype=jnp.int32)[None, :]).astype(
        jnp.int32
    )
    earlier = jnp.cumsum(onehot, axis=0) - onehot
    slot_index = jnp.sum(earlier * onehot, axis=1)
    target = (flat_expert * capacity + slot_index).reshape(tok_rows, top_count)
    places = jnp.arange(experts * capacity, dtype=jnp.int32)
    placing = jnp.sum(
        (target[:, :, None] == places[None, None, :]).astype(jnp.int32), axis=1
    ).astype(jnp.bfloat16)
    outgoing = lax.dot_general(
        placing, normed, (((0,), (0,)), ((), ())), preferred_element_type=jnp.float32
    ).astype(jnp.bfloat16)
    incoming = lax.all_to_all(
        outgoing.reshape(experts, capacity, portion_width),
        "fs",
        split_axis=0,
        concat_axis=0,
        tiled=True,
    )
    arrived = incoming.reshape(experts * capacity, portion_width)
    partials = (
        dense_rows(arrived, gate_refreshed[0]).astype(jnp.bfloat16),
        dense_rows(arrived, up_new[0]).astype(jnp.bfloat16),
        dense_rows(normed, shared_g).astype(jnp.bfloat16),
        dense_rows(normed, shared_u).astype(jnp.bfloat16),
    )
    gate_part, up_part, sgate_part, sup_part = (
        lax.psum_scatter(partials[0], "tp", scatter_dimension=1, tiled=True).astype(jnp.float32),
        lax.psum_scatter(partials[1], "tp", scatter_dimension=1, tiled=True).astype(jnp.float32),
        lax.psum_scatter(partials[2], "tp", scatter_dimension=1, tiled=True).astype(jnp.float32),
        lax.psum_scatter(partials[3], "tp", scatter_dimension=1, tiled=True).astype(jnp.float32),
    )
    hidden, shared_hidden = (
        lax.all_gather(
            (jax.nn.silu(gate_part) * up_part).astype(jnp.bfloat16), "tp", axis=1, tiled=True
        ),
        lax.all_gather(
            (jax.nn.silu(sgate_part) * sup_part).astype(jnp.bfloat16), "tp", axis=1, tiled=True
        ),
    )
    produced = jnp.dot(hidden, down_new[0], preferred_element_type=jnp.float32).astype(jnp.bfloat16)
    returned = lax.all_to_all(
        produced.reshape(experts, capacity, portion_width),
        "fs",
        split_axis=0,
        concat_axis=0,
        tiled=True,
    )
    picked = returned.reshape(experts * capacity, portion_width)[target]
    routed = jnp.sum(routing_weight[:, :, None] * picked.astype(jnp.float32), axis=1)
    shared_out = jnp.dot(shared_hidden, shared_d, preferred_element_type=jnp.float32)
    mixed = (routed + shared_out).astype(jnp.bfloat16)
    return (mixed, gate_refreshed, up_new, down_new, shared_g, shared_u, shared_d)


MESH = pl.DeviceIdType.MESH


def nearest_first(n):
    orders = [sorted(range(n), key=lambda s: (abs(s - f), s)) for f in range(n)]
    return [sum(orders[f][i] * n**f for f in range(n)) for i in range(n)]


def fused_kernel(
    n_fs, n_tp, top_count,
    tok_ref, meta_ref, gain_ref, eg_ref, eu_ref, ed_ref, sg_ref, su_ref, sd_ref,
    mixed_ref, wout_ref,
    wall, tokbuf, metabuf, ssown, ssbuf, scown, scbuf, mt, sct, part, rsbuf, hid, outf, outb, retbuf,
    tok_s, tok_r, meta_s, meta_r, ss_s, ss_r, sc_s, sc_r, rs_s, rs_r, ag_s, ag_r,
    ret_s, ret_r, we_s, we_r, ws_s, ws_r, ye_s, ye_r, ys_s, ys_r,
):
    g, f, t = lax.axis_index("grp"), lax.axis_index("fs"), lax.axis_index("tp")
    rows, width = tok_ref.shape
    experts, units = eg_ref.shape[0], eg_ref.shape[1]
    sub = rows // n_tp
    half = units // 2
    f32, bf16 = jnp.float32, jnp.bfloat16
    code = nearest_first(n_fs)

    def source(i):
        total = 0
        digits = code[i]
        picks = [(digits // n_fs**q) % n_fs for q in range(n_fs)]
        for q in range(n_fs):
            hit = 1 - jnp.minimum(1, jnp.abs(f - q))
            total = total + picks[q] * hit
        return total

    def at_fs(index):
        return (g, index, t)

    def at_tp(index):
        return (g, f, index)

    partner = (1 - g, f, t)

    def remote(src, dst, send, recv, device):
        return pltpu.make_async_remote_copy(
            src_ref=src, dst_ref=dst, send_sem=send, recv_sem=recv,
            device_id=device, device_id_type=MESH,
        )

    fs_others = [lax.rem(f + j, n_fs) for j in range(1, n_fs)]
    tp_others = [lax.rem(t + j, n_tp) for j in range(1, n_tp)]

    barrier = pltpu.get_barrier_semaphore()
    peers = [at_fs(d) for d in fs_others] + [at_tp(d) for d in tp_others] + [partner]
    for device in peers:
        pl.semaphore_signal(barrier, inc=1, device_id=device, device_id_type=MESH)
    pl.semaphore_wait(barrier, len(peers))

    def to_right(src, dst, send, recv):
        @pl.when(f < n_fs - 1)
        def _():
            remote(src, dst, send, recv, at_fs(f + 1)).start()

    def to_left(src, dst, send, recv):
        @pl.when(f > 0)
        def _():
            remote(src, dst, send, recv, at_fs(f - 1)).start()

    def onward(s, ref, send, recv):
        @pl.when((s < f) & (f < n_fs - 1))
        def _():
            remote(ref, ref, send.at[s, 0], recv.at[s], at_fs(f + 1)).start()

        @pl.when((s > f) & (f > 0))
        def _():
            remote(ref, ref, send.at[s, 1], recv.at[s], at_fs(f - 1)).start()

    def line_sends_done(refs, send, recv):
        for s in range(n_fs):
            ref = refs(s)

            @pl.when((f >= s) & (f < n_fs - 1))
            def _():
                remote(ref, ref, send.at[s, 0], recv.at[s], at_fs(f + 1)).wait_send()

            @pl.when((f <= s) & (f > 0))
            def _():
                remote(ref, ref, send.at[s, 1], recv.at[s], at_fs(f - 1)).wait_send()

    for go, way in ((to_right, 0), (to_left, 1)):
        go(meta_ref, metabuf.at[f], meta_s.at[f, way], meta_r.at[f])
        go(tok_ref, tokbuf.at[f], tok_s.at[f, way], tok_r.at[f])

    x = tok_ref[...].astype(f32)
    sq = x * x
    high = sq.astype(bf16)
    low = (sq - high.astype(f32)).astype(bf16)
    ones = jnp.ones((8, width), bf16)
    ssown[...] = jnp.zeros(ssown.shape, f32)
    ssown[:, 0:rows] = dense_rows(ones, high) + dense_rows(ones, low)
    for d in tp_others:
        remote(ssown, ssbuf.at[t], ss_s.at[d], ss_r.at[t], at_tp(d)).start()

    gain = gain_ref[...]
    for e in range(experts):
        wall[0, e] = (eg_ref[e] * gain).astype(bf16)
        wall[1, e] = (eu_ref[e] * gain).astype(bf16)
    wall[0, experts] = (sg_ref[...] * gain).astype(bf16)
    wall[1, experts] = (su_ref[...] * gain).astype(bf16)

    def transposed(row_ref):
        return jnp.transpose(row_ref[...])[0:rows]

    def forward_block(i, tokens, meta):
        mt[i] = transposed(meta)
        names = [mt[i, :, k : k + 1] for k in range(top_count)]
        columns = []
        for m in range(2):
            weight = wall[m].reshape((experts + 1) * units, width)
            sums = dense_rows(tokens[...], weight)
            for name in names:
                chosen = jnp.zeros((rows, units), f32)
                for e in range(experts):
                    chosen = jnp.where(name == float(e), sums[:, e * units : (e + 1) * units], chosen)
                columns.append(chosen)
            columns.append(sums[:, experts * units :])
        for c, column in enumerate(columns):
            part[i, :, :, c * units : (c + 1) * units] = column.astype(bf16).reshape(n_tp, sub, units)
        for d in tp_others:
            remote(part.at[i, d], rsbuf.at[i, t], rs_s.at[i, d], rs_r.at[i, t], at_tp(d)).start()

    def hidden_block(i, scale_row):
        sct[i] = transposed(scale_row)
        own_rows = pl.ds(pl.multiple_of(t * sub, 8), sub)
        scale = sct[i, own_rows, 0:1]
        weights = mt[i, own_rows, :]
        for d in tp_others:
            remote(part.at[i, d], rsbuf.at[i, d], rs_s.at[i, d], rs_r.at[i, d], at_tp(d)).wait_recv()
        total = part[i, t].astype(f32)
        for d in tp_others:
            total = total + rsbuf[i, d].astype(f32)
        total = total * scale
        kinds = top_count + 1
        for k in range(kinds):
            gate = total[:, k * units : (k + 1) * units]
            up = total[:, (kinds + k) * units : (kinds + k + 1) * units]
            value = jax.nn.silu(gate) * up
            if k < top_count:
                value = value * weights[:, top_count + k : top_count + k + 1]
            hid[i, t, :, k * units : (k + 1) * units] = value.astype(bf16)
        for d in tp_others:
            remote(hid.at[i, t], hid.at[i, t], ag_s.at[i, d], ag_r.at[i, t], at_tp(d)).start()

    def down_block(i):
        for d in tp_others:
            remote(hid.at[i, d], hid.at[i, d], ag_s.at[i, d], ag_r.at[i, d], at_tp(d)).wait_recv()
        values = hid[i].astype(f32).reshape(rows, (top_count + 1) * units)
        names = [mt[i, :, k : k + 1] for k in range(top_count)]
        spread = []
        for e in range(experts):
            chosen = jnp.zeros((rows, units), f32)
            for k, name in enumerate(names):
                chosen = jnp.where(name == float(e), values[:, k * units : (k + 1) * units], chosen)
            spread.append(chosen.astype(bf16))
        spread.append(values[:, top_count * units :].astype(bf16))
        weight = wall[2].reshape((experts + 1) * units, width)
        return jnp.dot(jnp.concatenate(spread, axis=1), weight, preferred_element_type=f32)

    def finish_block(i):
        product = down_block(i)
        if i == 0:
            outf[...] = product
        else:
            s = source(i)
            outb[i] = product.astype(bf16)
            remote(outb.at[i], retbuf.at[f], ret_s.at[i], ret_r.at[f], at_fs(s)).start()

    def token_block(i):
        s = source(i)
        remote(metabuf.at[s], metabuf.at[s], meta_s.at[s, 0], meta_r.at[s], partner).wait_recv()
        onward(s, metabuf.at[s], meta_s, meta_r)
        remote(tokbuf.at[s], tokbuf.at[s], tok_s.at[s, 0], tok_r.at[s], partner).wait_recv()
        onward(s, tokbuf.at[s], tok_s, tok_r)

    def scale_block(i):
        s = source(i)
        remote(scown, scbuf.at[s], sc_s.at[s], sc_r.at[s], partner).wait_recv()
        return scbuf.at[s]

    forward_block(0, tok_ref, meta_ref)
    squares = ssown[...]
    for d in tp_others:
        remote(ssown, ssbuf.at[d], ss_s.at[d], ss_r.at[d], at_tp(d)).wait_recv()
        squares = squares + ssbuf[d]
    scown[...] = lax.rsqrt(squares / (width * n_tp) + norm_eps)
    for d in fs_others:
        remote(scown, scbuf.at[f], sc_s.at[d], sc_r.at[f], at_fs(d)).start()
    for e in range(experts):
        wall[2, e] = ed_ref[e].astype(bf16)
    wall[2, experts] = sd_ref[...].astype(bf16)

    token_block(1)
    forward_block(1, tokbuf.at[source(1)], metabuf.at[source(1)])
    hidden_block(0, scown)
    for i in range(2, n_fs):
        token_block(i)
        if i == n_fs - 1:
            mine = pl.ds(pl.multiple_of(g * half, 16), half)
            for way, go in ((0, to_right), (1, to_left)):
                go(wall.at[:, experts, mine], wout_ref.at[1, :, f, g], ws_s.at[f, way], ws_r.at[f])
            for d in fs_others:
                remote(
                    wall.at[:, d, mine], wout_ref.at[0, :, f, g], we_s.at[d], we_r.at[f], at_fs(d)
                ).start()
        forward_block(i, tokbuf.at[source(i)], metabuf.at[source(i)])
        hidden_block(i - 1, scale_block(i - 1))
        finish_block(i - 2)
    for h in range(2):
        wout_ref[0, :, f, h] = wall[:, f, h * half : (h + 1) * half]
        wout_ref[1, :, f, h] = wall[:, experts, h * half : (h + 1) * half]
    hidden_block(n_fs - 1, scale_block(n_fs - 1))
    finish_block(n_fs - 2)
    finish_block(n_fs - 1)

    for i in range(1, n_fs):
        s = source(i)
        shared, routed = wout_ref.at[1, :, s, g], wout_ref.at[0, :, s, g]
        remote(shared, shared, ws_s.at[s, 0], ws_r.at[s], partner).wait_recv()
        onward(s, shared, ws_s, ws_r)
        remote(shared, shared, ys_s.at[s], ys_r.at[s], partner).start()
        remote(routed, routed, we_s.at[s], we_r.at[s], partner).wait_recv()
        remote(routed, routed, ye_s.at[s], ye_r.at[s], partner).start()

    total = outf[...]
    for d in fs_others:
        remote(retbuf.at[d], retbuf.at[d], ret_s.at[1], ret_r.at[d], partner).wait_recv()
        total = total + retbuf[d].astype(f32)
    mixed_ref[...] = total.astype(bf16)

    for d in fs_others:
        shared, routed = wout_ref.at[1, :, d, 1 - g], wout_ref.at[0, :, d, 1 - g]
        remote(shared, shared, ys_s.at[d], ys_r.at[d], partner).wait_recv()
        remote(routed, routed, ye_s.at[d], ye_r.at[d], partner).wait_recv()

    line_sends_done(lambda s: metabuf.at[s], meta_s, meta_r)
    line_sends_done(lambda s: tokbuf.at[s], tok_s, tok_r)
    line_sends_done(lambda s: wout_ref.at[1, :, s, g], ws_s, ws_r)
    for d in tp_others:
        remote(ssown, ssbuf.at[t], ss_s.at[d], ss_r.at[t], at_tp(d)).wait_send()
        for i in range(n_fs):
            remote(part.at[i, d], rsbuf.at[i, t], rs_s.at[i, d], rs_r.at[i, t], at_tp(d)).wait_send()
            remote(hid.at[i, t], hid.at[i, t], ag_s.at[i, d], ag_r.at[i, t], at_tp(d)).wait_send()
    for j, d in enumerate(fs_others):
        remote(scown, scbuf.at[f], sc_s.at[d], sc_r.at[f], at_fs(d)).wait_send()
        remote(outb.at[j + 1], retbuf.at[f], ret_s.at[j + 1], ret_r.at[f], at_fs(d)).wait_send()
        shared, routed = wout_ref.at[1, :, d, g], wout_ref.at[0, :, d, g]
        remote(routed, routed, we_s.at[d], we_r.at[f], at_fs(d)).wait_send()
        remote(shared, shared, ys_s.at[d], ys_r.at[d], partner).wait_send()
        remote(routed, routed, ye_s.at[d], ye_r.at[d], partner).wait_send()


def per_device_fused(
    tokens,
    routes,
    routing_weight,
    norm_gain_vector,
    expert_gate,
    expert_up,
    expert_down,
    shared_gate,
    shared_up,
    shared_down,
):
    n_fs, n_tp = lax.axis_size("fs"), lax.axis_size("tp")
    rows, width = tokens.shape
    experts, units, _ = expert_gate.shape
    top_count = routes.shape[1]
    sub, half = rows // n_tp, units // 2
    meta_rows = -(-2 * top_count // 8) * 8
    lanes = -(-rows // 128) * 128
    meta = jnp.concatenate([routes.astype(jnp.float32), routing_weight], axis=1).T
    meta = jnp.pad(meta, ((0, meta_rows - 2 * top_count), (0, lanes - rows)))
    f32, bf16 = jnp.float32, jnp.bfloat16
    kinds = top_count + 1
    dma = pltpu.SemaphoreType.DMA
    vmem = pl.BlockSpec(memory_space=pltpu.VMEM)
    mixed, served = pl.pallas_call(
        functools.partial(fused_kernel, n_fs, n_tp, top_count),
        out_shape=(
            jax.ShapeDtypeStruct((rows, width), bf16),
            jax.ShapeDtypeStruct((2, 3, n_fs, 2, half, width), bf16),
        ),
        in_specs=[vmem] * 9,
        out_specs=(vmem, vmem),
        scratch_shapes=[
            pltpu.VMEM((3, experts + 1, units, width), bf16),
            pltpu.VMEM((n_fs, rows, width), bf16),
            pltpu.VMEM((n_fs, meta_rows, lanes), f32),
            pltpu.VMEM((8, lanes), f32),
            pltpu.VMEM((n_tp, 8, lanes), f32),
            pltpu.VMEM((8, lanes), f32),
            pltpu.VMEM((n_fs, 8, lanes), f32),
            pltpu.VMEM((n_fs, rows, meta_rows), f32),
            pltpu.VMEM((n_fs, rows, 8), f32),
            pltpu.VMEM((n_fs, n_tp, sub, 2 * kinds * units), bf16),
            pltpu.VMEM((n_fs, n_tp, sub, 2 * kinds * units), bf16),
            pltpu.VMEM((n_fs, n_tp, sub, kinds * units), bf16),
            pltpu.VMEM((rows, width), f32),
            pltpu.VMEM((n_fs, rows, width), bf16),
            pltpu.VMEM((n_fs, rows, width), bf16),
            dma((n_fs, 2)), dma((n_fs,)),
            dma((n_fs, 2)), dma((n_fs,)),
            dma((n_tp,)), dma((n_tp,)),
            dma((n_fs,)), dma((n_fs,)),
            dma((n_fs, n_tp)), dma((n_fs, n_tp)),
            dma((n_fs, n_tp)), dma((n_fs, n_tp)),
            dma((n_fs,)), dma((n_fs,)),
            dma((n_fs,)), dma((n_fs,)),
            dma((n_fs, 2)), dma((n_fs,)),
            dma((n_fs,)), dma((n_fs,)),
            dma((n_fs,)), dma((n_fs,)),
        ],
        compiler_params=pltpu.CompilerParams(
            collective_id=0, has_side_effects=True, vmem_limit_bytes=60 * 1024 * 1024
        ),
        name="hand_over_and_layer",
    )(
        tokens, meta, norm_gain_vector[None, :],
        expert_gate, expert_up, expert_down, shared_gate, shared_up, shared_down,
    )
    served = served.reshape(2, 3, n_fs * units, width)
    return (
        mixed,
        served[0, 0][None], served[0, 1][None], served[0, 2][None],
        served[1, 0], served[1, 1], served[1, 2],
    )


def per_device(tokens, routes, routing_weight, norm_gain_vector, *weights):
    experts, units, width = weights[0].shape
    rows, n_fs, n_tp = tokens.shape[0], lax.axis_size("fs"), lax.axis_size("tp")
    whole_tiles = units % 128 == 0 and width % 128 == 0 and rows % (16 * n_tp) == 0
    fits = (experts + 1) * units * width <= 2**20 and n_fs <= 4 and n_tp <= 4
    chosen = per_device_plain
    if whole_tiles and fits and experts == n_fs and lax.axis_size("grp") == 2 and n_fs > 2:
        chosen = per_device_fused
    return chosen(tokens, routes, routing_weight, norm_gain_vector, *weights)


def solution(mesh):
    return jax.shard_map(
        per_device,
        mesh=mesh,
        in_specs=(
            P(("grp", "fs"), "tp"),
            P(("grp", "fs"), None),
            P(("grp", "fs"), None),
            P("tp"),
            P(None, "fs", "tp"),
            P(None, "fs", "tp"),
            P(None, "fs", "tp"),
            P("fs", "tp"),
            P("fs", "tp"),
            P("fs", "tp"),
        ),
        out_specs=(
            P(("grp", "fs"), "tp"),
            P(("grp", "fs"), None, "tp"),
            P(("grp", "fs"), None, "tp"),
            P(("grp", "fs"), None, "tp"),
            P("grp", "tp"),
            P("grp", "tp"),
            P("grp", "tp"),
        ),
        check_vma=False,
    )
```

```python
import functools

import jax
import jax.numpy as jnp
from jax import lax
from jax.experimental import pallas as pl
from jax.experimental.pallas import tpu as pltpu
from jax.sharding import PartitionSpec as P

norm_eps = 1e-06


def dense_rows(rows, weight):
    return lax.dot_general(
        rows, weight, (((1,), (1,)), ((), ())), preferred_element_type=jnp.float32
    )


def per_device_plain(
    tokens,
    routes,
    routing_weight,
    norm_gain_vector,
    expert_gate,
    expert_up,
    expert_down,
    shared_gate,
    shared_up,
    shared_down,
):
    tok_rows, portion_width = tokens.shape
    model_width = portion_width * lax.axis_size("tp")
    experts = expert_gate.shape[0]
    top_count = routes.shape[1]
    capacity = tok_rows * top_count * 7 // (6 * experts)
    gate_round = (expert_gate * norm_gain_vector[None, None, :]).astype(jnp.bfloat16)
    up_round = (expert_up * norm_gain_vector[None, None, :]).astype(jnp.bfloat16)
    down_round = expert_down.astype(jnp.bfloat16)
    gate_refreshed, up_new, down_new = (
        lax.all_to_all(gate_round, "fs", split_axis=0, concat_axis=1, tiled=True),
        lax.all_to_all(up_round, "fs", split_axis=0, concat_axis=1, tiled=True),
        lax.all_to_all(down_round, "fs", split_axis=0, concat_axis=1, tiled=True),
    )
    shared_g, shared_u, shared_d = (
        lax.all_gather(
            (shared_gate * norm_gain_vector[None, :]).astype(jnp.bfloat16), "fs", axis=0, tiled=True
        ),
        lax.all_gather(
            (shared_up * norm_gain_vector[None, :]).astype(jnp.bfloat16), "fs", axis=0, tiled=True
        ),
        lax.all_gather(shared_down.astype(jnp.bfloat16), "fs", axis=0, tiled=True),
    )
    values = tokens.astype(jnp.float32)
    totals = lax.psum(jnp.sum(values * values, axis=1), "tp")
    normed = (values * lax.rsqrt(totals / model_width + norm_eps)[:, None]).astype(jnp.bfloat16)
    flat_expert = routes.reshape(-1)
    onehot = (flat_expert[:, None] == jnp.arange(experts, dtype=jnp.int32)[None, :]).astype(
        jnp.int32
    )
    earlier = jnp.cumsum(onehot, axis=0) - onehot
    slot_index = jnp.sum(earlier * onehot, axis=1)
    target = (flat_expert * capacity + slot_index).reshape(tok_rows, top_count)
    places = jnp.arange(experts * capacity, dtype=jnp.int32)
    placing = jnp.sum(
        (target[:, :, None] == places[None, None, :]).astype(jnp.int32), axis=1
    ).astype(jnp.bfloat16)
    outgoing = lax.dot_general(
        placing, normed, (((0,), (0,)), ((), ())), preferred_element_type=jnp.float32
    ).astype(jnp.bfloat16)
    incoming = lax.all_to_all(
        outgoing.reshape(experts, capacity, portion_width),
        "fs",
        split_axis=0,
        concat_axis=0,
        tiled=True,
    )
    arrived = incoming.reshape(experts * capacity, portion_width)
    partials = (
        dense_rows(arrived, gate_refreshed[0]).astype(jnp.bfloat16),
        dense_rows(arrived, up_new[0]).astype(jnp.bfloat16),
        dense_rows(normed, shared_g).astype(jnp.bfloat16),
        dense_rows(normed, shared_u).astype(jnp.bfloat16),
    )
    gate_part, up_part, sgate_part, sup_part = (
        lax.psum_scatter(partials[0], "tp", scatter_dimension=1, tiled=True).astype(jnp.float32),
        lax.psum_scatter(partials[1], "tp", scatter_dimension=1, tiled=True).astype(jnp.float32),
        lax.psum_scatter(partials[2], "tp", scatter_dimension=1, tiled=True).astype(jnp.float32),
        lax.psum_scatter(partials[3], "tp", scatter_dimension=1, tiled=True).astype(jnp.float32),
    )
    hidden, shared_hidden = (
        lax.all_gather(
            (jax.nn.silu(gate_part) * up_part).astype(jnp.bfloat16), "tp", axis=1, tiled=True
        ),
        lax.all_gather(
            (jax.nn.silu(sgate_part) * sup_part).astype(jnp.bfloat16), "tp", axis=1, tiled=True
        ),
    )
    produced = jnp.dot(hidden, down_new[0], preferred_element_type=jnp.float32).astype(jnp.bfloat16)
    returned = lax.all_to_all(
        produced.reshape(experts, capacity, portion_width),
        "fs",
        split_axis=0,
        concat_axis=0,
        tiled=True,
    )
    picked = returned.reshape(experts * capacity, portion_width)[target]
    routed = jnp.sum(routing_weight[:, :, None] * picked.astype(jnp.float32), axis=1)
    shared_out = jnp.dot(shared_hidden, shared_d, preferred_element_type=jnp.float32)
    mixed = (routed + shared_out).astype(jnp.bfloat16)
    return (mixed, gate_refreshed, up_new, down_new, shared_g, shared_u, shared_d)


MESH = pl.DeviceIdType.MESH


def nearest_first(n):
    orders = [sorted(range(n), key=lambda s: (abs(s - f), s)) for f in range(n)]
    return [sum(orders[f][i] * n**f for f in range(n)) for i in range(n)]


def fused_kernel(
    n_fs, n_tp, top_count,
    tok_ref, routes_ref, weight_ref, gain_ref, eg_ref, eu_ref, ed_ref, sg_ref, su_ref, sd_ref,
    mixed_ref, wout_ref,
    wall, tokbuf, meta_ref, metabuf, ssown, ssbuf, scown, scbuf, mt, sct, part, rsbuf, hid, outf, outb, retbuf,
    tok_s, tok_r, meta_s, meta_r, ss_s, ss_r, sc_s, sc_r, rs_s, rs_r, ag_s, ag_r,
    ret_s, ret_r, we_s, we_r, ws_s, ws_r, ye_s, ye_r, ys_s, ys_r,
):
    g, f, t = lax.axis_index("grp"), lax.axis_index("fs"), lax.axis_index("tp")
    rows, width = tok_ref.shape
    experts, units = eg_ref.shape[0], eg_ref.shape[1]
    sub = rows // n_tp
    half = units // 2
    f32, bf16 = jnp.float32, jnp.bfloat16
    code = nearest_first(n_fs)

    def source(i):
        total = 0
        digits = code[i]
        picks = [(digits // n_fs**q) % n_fs for q in range(n_fs)]
        for q in range(n_fs):
            hit = 1 - jnp.minimum(1, jnp.abs(f - q))
            total = total + picks[q] * hit
        return total

    def at_fs(index):
        return (g, index, t)

    def at_tp(index):
        return (g, f, index)

    partner = (1 - g, f, t)

    def remote(src, dst, send, recv, device):
        return pltpu.make_async_remote_copy(
            src_ref=src, dst_ref=dst, send_sem=send, recv_sem=recv,
            device_id=device, device_id_type=MESH,
        )

    fs_others = [lax.rem(f + j, n_fs) for j in range(1, n_fs)]
    tp_others = [lax.rem(t + j, n_tp) for j in range(1, n_tp)]

    barrier = pltpu.get_barrier_semaphore()
    peers = [at_fs(d) for d in fs_others] + [at_tp(d) for d in tp_others] + [partner]
    for device in peers:
        pl.semaphore_signal(barrier, inc=1, device_id=device, device_id_type=MESH)
    pl.semaphore_wait(barrier, len(peers))

    def to_right(src, dst, send, recv):
        @pl.when(f < n_fs - 1)
        def _():
            remote(src, dst, send, recv, at_fs(f + 1)).start()

    def to_left(src, dst, send, recv):
        @pl.when(f > 0)
        def _():
            remote(src, dst, send, recv, at_fs(f - 1)).start()

    def onward(s, ref, send, recv):
        @pl.when((s < f) & (f < n_fs - 1))
        def _():
            remote(ref, ref, send.at[s, 0], recv.at[s], at_fs(f + 1)).start()

        @pl.when((s > f) & (f > 0))
        def _():
            remote(ref, ref, send.at[s, 1], recv.at[s], at_fs(f - 1)).start()

    def line_sends_done(refs, send, recv):
        for s in range(n_fs):
            ref = refs(s)

            @pl.when((f >= s) & (f < n_fs - 1))
            def _():
                remote(ref, ref, send.at[s, 0], recv.at[s], at_fs(f + 1)).wait_send()

            @pl.when((f <= s) & (f > 0))
            def _():
                remote(ref, ref, send.at[s, 1], recv.at[s], at_fs(f - 1)).wait_send()

    meta_ref[...] = jnp.zeros(meta_ref.shape, f32)
    meta_ref[0:top_count, 0:rows] = routes_ref[...].astype(f32)
    meta_ref[top_count : 2 * top_count, 0:rows] = weight_ref[...]
    for go, way in ((to_right, 0), (to_left, 1)):
        go(meta_ref, metabuf.at[f], meta_s.at[f, way], meta_r.at[f])
        go(tok_ref, tokbuf.at[f], tok_s.at[f, way], tok_r.at[f])

    x = tok_ref[...].astype(f32)
    sq = x * x
    high = sq.astype(bf16)
    low = (sq - high.astype(f32)).astype(bf16)
    ones = jnp.ones((8, width), bf16)
    ssown[...] = jnp.zeros(ssown.shape, f32)
    ssown[:, 0:rows] = dense_rows(ones, high) + dense_rows(ones, low)
    for d in tp_others:
        remote(ssown, ssbuf.at[t], ss_s.at[d], ss_r.at[t], at_tp(d)).start()

    gain = gain_ref[...]
    for e in range(experts):
        wall[0, e] = (eg_ref[e] * gain).astype(bf16)
        wall[1, e] = (eu_ref[e] * gain).astype(bf16)
    wall[0, experts] = (sg_ref[...] * gain).astype(bf16)
    wall[1, experts] = (su_ref[...] * gain).astype(bf16)

    def transposed(row_ref):
        return jnp.transpose(row_ref[...])[0:rows]

    def forward_block(i, tokens, meta):
        mt[i] = transposed(meta)
        names = [mt[i, :, k : k + 1] for k in range(top_count)]
        columns = []
        for m in range(2):
            weight = wall[m].reshape((experts + 1) * units, width)
            sums = dense_rows(tokens[...], weight)
            for name in names:
                chosen = jnp.zeros((rows, units), f32)
                for e in range(experts):
                    chosen = jnp.where(name == float(e), sums[:, e * units : (e + 1) * units], chosen)
                columns.append(chosen)
            columns.append(sums[:, experts * units :])
        for c, column in enumerate(columns):
            part[i, :, :, c * units : (c + 1) * units] = column.astype(bf16).reshape(n_tp, sub, units)
        for d in tp_others:
            remote(part.at[i, d], rsbuf.at[i, t], rs_s.at[i, d], rs_r.at[i, t], at_tp(d)).start()

    def hidden_block(i, scale_row):
        sct[i] = transposed(scale_row)
        own_rows = pl.ds(pl.multiple_of(t * sub, 8), sub)
        scale = sct[i, own_rows, 0:1]
        weights = mt[i, own_rows, :]
        for d in tp_others:
            remote(part.at[i, d], rsbuf.at[i, d], rs_s.at[i, d], rs_r.at[i, d], at_tp(d)).wait_recv()
        total = part[i, t].astype(f32)
        for d in tp_others:
            total = total + rsbuf[i, d].astype(f32)
        total = total * scale
        kinds = top_count + 1
        for k in range(kinds):
            gate = total[:, k * units : (k + 1) * units]
            up = total[:, (kinds + k) * units : (kinds + k + 1) * units]
            value = jax.nn.silu(gate) * up
            if k < top_count:
                value = value * weights[:, top_count + k : top_count + k + 1]
            hid[i, t, :, k * units : (k + 1) * units] = value.astype(bf16)
        for d in tp_others:
            remote(hid.at[i, t], hid.at[i, t], ag_s.at[i, d], ag_r.at[i, t], at_tp(d)).start()

    def down_block(i):
        for d in tp_others:
            remote(hid.at[i, d], hid.at[i, d], ag_s.at[i, d], ag_r.at[i, d], at_tp(d)).wait_recv()
        values = hid[i].astype(f32).reshape(rows, (top_count + 1) * units)
        names = [mt[i, :, k : k + 1] for k in range(top_count)]
        spread = []
        for e in range(experts):
            chosen = jnp.zeros((rows, units), f32)
            for k, name in enumerate(names):
                chosen = jnp.where(name == float(e), values[:, k * units : (k + 1) * units], chosen)
            spread.append(chosen.astype(bf16))
        spread.append(values[:, top_count * units :].astype(bf16))
        weight = wall[2].reshape((experts + 1) * units, width)
        return jnp.dot(jnp.concatenate(spread, axis=1), weight, preferred_element_type=f32)

    def finish_block(i):
        product = down_block(i)
        if i == 0:
            outf[...] = product
        else:
            s = source(i)
            outb[i] = product.astype(bf16)
            remote(outb.at[i], retbuf.at[f], ret_s.at[i], ret_r.at[f], at_fs(s)).start()

    def token_block(i):
        s = source(i)
        remote(metabuf.at[s], metabuf.at[s], meta_s.at[s, 0], meta_r.at[s], partner).wait_recv()
        onward(s, metabuf.at[s], meta_s, meta_r)
        remote(tokbuf.at[s], tokbuf.at[s], tok_s.at[s, 0], tok_r.at[s], partner).wait_recv()
        onward(s, tokbuf.at[s], tok_s, tok_r)

    def scale_block(i):
        s = source(i)
        remote(scown, scbuf.at[s], sc_s.at[s], sc_r.at[s], partner).wait_recv()
        return scbuf.at[s]

    for e in range(experts):
        wall[2, e] = ed_ref[e].astype(bf16)
    wall[2, experts] = sd_ref[...].astype(bf16)

    mine = pl.ds(pl.multiple_of(g * half, 16), half)
    for way, go in ((0, to_right), (1, to_left)):
        go(wall.at[:, experts, mine], wout_ref.at[1, :, f, g], ws_s.at[f, way], ws_r.at[f])

    def give_expert(i):
        d = source(i)
        remote(
            wall.at[:, d, mine], wout_ref.at[0, :, f, g], we_s.at[d], we_r.at[f], at_fs(d)
        ).start()

    def pass_shared(i):
        s = source(i)
        shared = wout_ref.at[1, :, s, g]
        remote(shared, shared, ws_s.at[s, 0], ws_r.at[s], partner).wait_recv()
        onward(s, shared, ws_s, ws_r)
        remote(shared, shared, ys_s.at[s], ys_r.at[s], partner).start()

    def pass_routed(i):
        s = source(i)
        routed = wout_ref.at[0, :, s, g]
        remote(routed, routed, we_s.at[s], we_r.at[s], partner).wait_recv()
        remote(routed, routed, ye_s.at[s], ye_r.at[s], partner).start()

    forward_block(0, tok_ref, meta_ref)
    squares = ssown[...]
    for d in tp_others:
        remote(ssown, ssbuf.at[d], ss_s.at[d], ss_r.at[d], at_tp(d)).wait_recv()
        squares = squares + ssbuf[d]
    scown[...] = lax.rsqrt(squares / (width * n_tp) + norm_eps)
    for d in fs_others:
        remote(scown, scbuf.at[f], sc_s.at[d], sc_r.at[f], at_fs(d)).start()
    for h in range(2):
        wout_ref[0, :, f, h] = wall[:, f, h * half : (h + 1) * half]
        wout_ref[1, :, f, h] = wall[:, experts, h * half : (h + 1) * half]

    for i in range(1, n_fs):
        token_block(i)
        give_expert(i)
        forward_block(i, tokbuf.at[source(i)], metabuf.at[source(i)])
        hidden_block(i - 1, scown if i == 1 else scale_block(i - 1))
        if i >= 2:
            finish_block(i - 2)
            pass_shared(i - 1)
    pass_routed(1)
    hidden_block(n_fs - 1, scale_block(n_fs - 1))
    finish_block(n_fs - 2)
    finish_block(n_fs - 1)
    pass_shared(n_fs - 1)
    for i in range(2, n_fs):
        pass_routed(i)

    total = outf[...]
    for d in fs_others:
        remote(retbuf.at[d], retbuf.at[d], ret_s.at[1], ret_r.at[d], partner).wait_recv()
        total = total + retbuf[d].astype(f32)
    mixed_ref[...] = total.astype(bf16)

    for d in fs_others:
        shared, routed = wout_ref.at[1, :, d, 1 - g], wout_ref.at[0, :, d, 1 - g]
        remote(shared, shared, ys_s.at[d], ys_r.at[d], partner).wait_recv()
        remote(routed, routed, ye_s.at[d], ye_r.at[d], partner).wait_recv()

    line_sends_done(lambda s: metabuf.at[s], meta_s, meta_r)
    line_sends_done(lambda s: tokbuf.at[s], tok_s, tok_r)
    line_sends_done(lambda s: wout_ref.at[1, :, s, g], ws_s, ws_r)
    for d in tp_others:
        remote(ssown, ssbuf.at[t], ss_s.at[d], ss_r.at[t], at_tp(d)).wait_send()
        for i in range(n_fs):
            remote(part.at[i, d], rsbuf.at[i, t], rs_s.at[i, d], rs_r.at[i, t], at_tp(d)).wait_send()
            remote(hid.at[i, t], hid.at[i, t], ag_s.at[i, d], ag_r.at[i, t], at_tp(d)).wait_send()
    for j, d in enumerate(fs_others):
        remote(scown, scbuf.at[f], sc_s.at[d], sc_r.at[f], at_fs(d)).wait_send()
        remote(outb.at[j + 1], retbuf.at[f], ret_s.at[j + 1], ret_r.at[f], at_fs(d)).wait_send()
        shared, routed = wout_ref.at[1, :, d, g], wout_ref.at[0, :, d, g]
        remote(routed, routed, we_s.at[d], we_r.at[f], at_fs(d)).wait_send()
        remote(shared, shared, ys_s.at[d], ys_r.at[d], partner).wait_send()
        remote(routed, routed, ye_s.at[d], ye_r.at[d], partner).wait_send()


def per_device_fused(
    tokens,
    routes,
    routing_weight,
    norm_gain_vector,
    expert_gate,
    expert_up,
    expert_down,
    shared_gate,
    shared_up,
    shared_down,
):
    n_fs, n_tp = lax.axis_size("fs"), lax.axis_size("tp")
    rows, width = tokens.shape
    experts, units, _ = expert_gate.shape
    top_count = routes.shape[1]
    sub, half = rows // n_tp, units // 2
    meta_rows = -(-2 * top_count // 8) * 8
    lanes = -(-rows // 128) * 128
    f32, bf16 = jnp.float32, jnp.bfloat16
    kinds = top_count + 1
    dma = pltpu.SemaphoreType.DMA
    vmem = pl.BlockSpec(memory_space=pltpu.VMEM)
    mixed, served = pl.pallas_call(
        functools.partial(fused_kernel, n_fs, n_tp, top_count),
        out_shape=(
            jax.ShapeDtypeStruct((rows, width), bf16),
            jax.ShapeDtypeStruct((2, 3, n_fs, 2, half, width), bf16),
        ),
        in_specs=[vmem] * 10,
        out_specs=(vmem, vmem),
        scratch_shapes=[
            pltpu.VMEM((3, experts + 1, units, width), bf16),
            pltpu.VMEM((n_fs, rows, width), bf16),
            pltpu.VMEM((meta_rows, lanes), f32),
            pltpu.VMEM((n_fs, meta_rows, lanes), f32),
            pltpu.VMEM((8, lanes), f32),
            pltpu.VMEM((n_tp, 8, lanes), f32),
            pltpu.VMEM((8, lanes), f32),
            pltpu.VMEM((n_fs, 8, lanes), f32),
            pltpu.VMEM((n_fs, rows, meta_rows), f32),
            pltpu.VMEM((n_fs, rows, 8), f32),
            pltpu.VMEM((n_fs, n_tp, sub, 2 * kinds * units), bf16),
            pltpu.VMEM((n_fs, n_tp, sub, 2 * kinds * units), bf16),
            pltpu.VMEM((n_fs, n_tp, sub, kinds * units), bf16),
            pltpu.VMEM((rows, width), f32),
            pltpu.VMEM((n_fs, rows, width), bf16),
            pltpu.VMEM((n_fs, rows, width), bf16),
            dma((n_fs, 2)), dma((n_fs,)),
            dma((n_fs, 2)), dma((n_fs,)),
            dma((n_tp,)), dma((n_tp,)),
            dma((n_fs,)), dma((n_fs,)),
            dma((n_fs, n_tp)), dma((n_fs, n_tp)),
            dma((n_fs, n_tp)), dma((n_fs, n_tp)),
            dma((n_fs,)), dma((n_fs,)),
            dma((n_fs,)), dma((n_fs,)),
            dma((n_fs, 2)), dma((n_fs,)),
            dma((n_fs,)), dma((n_fs,)),
            dma((n_fs,)), dma((n_fs,)),
        ],
        compiler_params=pltpu.CompilerParams(
            collective_id=0, has_side_effects=True, vmem_limit_bytes=60 * 1024 * 1024
        ),
        name="hand_over_and_layer",
    )(
        tokens, routes.T, routing_weight.T, norm_gain_vector[None, :],
        expert_gate, expert_up, expert_down, shared_gate, shared_up, shared_down,
    )
    served = served.reshape(2, 3, n_fs * units, width)
    return (
        mixed,
        served[0, 0][None], served[0, 1][None], served[0, 2][None],
        served[1, 0], served[1, 1], served[1, 2],
    )


def per_device(tokens, routes, routing_weight, norm_gain_vector, *weights):
    experts, units, width = weights[0].shape
    rows, n_fs, n_tp = tokens.shape[0], lax.axis_size("fs"), lax.axis_size("tp")
    whole_tiles = units % 128 == 0 and width % 128 == 0 and rows % (16 * n_tp) == 0
    fits = (experts + 1) * units * width <= 2**20 and n_fs <= 4 and n_tp <= 4
    chosen = per_device_plain
    if whole_tiles and fits and experts == n_fs and lax.axis_size("grp") == 2 and n_fs > 2:
        chosen = per_device_fused
    return chosen(tokens, routes, routing_weight, norm_gain_vector, *weights)


def solution(mesh):
    return jax.shard_map(
        per_device,
        mesh=mesh,
        in_specs=(
            P(("grp", "fs"), "tp"),
            P(("grp", "fs"), None),
            P(("grp", "fs"), None),
            P("tp"),
            P(None, "fs", "tp"),
            P(None, "fs", "tp"),
            P(None, "fs", "tp"),
            P("fs", "tp"),
            P("fs", "tp"),
            P("fs", "tp"),
        ),
        out_specs=(
            P(("grp", "fs"), "tp"),
            P(("grp", "fs"), None, "tp"),
            P(("grp", "fs"), None, "tp"),
            P(("grp", "fs"), None, "tp"),
            P("grp", "tp"),
            P("grp", "tp"),
            P("grp", "tp"),
        ),
        check_vma=False,
    )
```

```python
import functools

import jax
import jax.numpy as jnp
from jax import lax
from jax.experimental import pallas as pl
from jax.experimental.pallas import tpu as pltpu
from jax.sharding import PartitionSpec as P

norm_eps = 1e-06


def dense_rows(rows, weight):
    return lax.dot_general(
        rows, weight, (((1,), (1,)), ((), ())), preferred_element_type=jnp.float32
    )


def per_device_plain(
    tokens,
    routes,
    routing_weight,
    norm_gain_vector,
    expert_gate,
    expert_up,
    expert_down,
    shared_gate,
    shared_up,
    shared_down,
):
    tok_rows, portion_width = tokens.shape
    model_width = portion_width * lax.axis_size("tp")
    experts = expert_gate.shape[0]
    top_count = routes.shape[1]
    capacity = tok_rows * top_count * 7 // (6 * experts)
    gate_round = (expert_gate * norm_gain_vector[None, None, :]).astype(jnp.bfloat16)
    up_round = (expert_up * norm_gain_vector[None, None, :]).astype(jnp.bfloat16)
    down_round = expert_down.astype(jnp.bfloat16)
    gate_refreshed, up_new, down_new = (
        lax.all_to_all(gate_round, "fs", split_axis=0, concat_axis=1, tiled=True),
        lax.all_to_all(up_round, "fs", split_axis=0, concat_axis=1, tiled=True),
        lax.all_to_all(down_round, "fs", split_axis=0, concat_axis=1, tiled=True),
    )
    shared_g, shared_u, shared_d = (
        lax.all_gather(
            (shared_gate * norm_gain_vector[None, :]).astype(jnp.bfloat16), "fs", axis=0, tiled=True
        ),
        lax.all_gather(
            (shared_up * norm_gain_vector[None, :]).astype(jnp.bfloat16), "fs", axis=0, tiled=True
        ),
        lax.all_gather(shared_down.astype(jnp.bfloat16), "fs", axis=0, tiled=True),
    )
    values = tokens.astype(jnp.float32)
    totals = lax.psum(jnp.sum(values * values, axis=1), "tp")
    normed = (values * lax.rsqrt(totals / model_width + norm_eps)[:, None]).astype(jnp.bfloat16)
    flat_expert = routes.reshape(-1)
    onehot = (flat_expert[:, None] == jnp.arange(experts, dtype=jnp.int32)[None, :]).astype(
        jnp.int32
    )
    earlier = jnp.cumsum(onehot, axis=0) - onehot
    slot_index = jnp.sum(earlier * onehot, axis=1)
    target = (flat_expert * capacity + slot_index).reshape(tok_rows, top_count)
    places = jnp.arange(experts * capacity, dtype=jnp.int32)
    placing = jnp.sum(
        (target[:, :, None] == places[None, None, :]).astype(jnp.int32), axis=1
    ).astype(jnp.bfloat16)
    outgoing = lax.dot_general(
        placing, normed, (((0,), (0,)), ((), ())), preferred_element_type=jnp.float32
    ).astype(jnp.bfloat16)
    incoming = lax.all_to_all(
        outgoing.reshape(experts, capacity, portion_width),
        "fs",
        split_axis=0,
        concat_axis=0,
        tiled=True,
    )
    arrived = incoming.reshape(experts * capacity, portion_width)
    partials = (
        dense_rows(arrived, gate_refreshed[0]).astype(jnp.bfloat16),
        dense_rows(arrived, up_new[0]).astype(jnp.bfloat16),
        dense_rows(normed, shared_g).astype(jnp.bfloat16),
        dense_rows(normed, shared_u).astype(jnp.bfloat16),
    )
    gate_part, up_part, sgate_part, sup_part = (
        lax.psum_scatter(partials[0], "tp", scatter_dimension=1, tiled=True).astype(jnp.float32),
        lax.psum_scatter(partials[1], "tp", scatter_dimension=1, tiled=True).astype(jnp.float32),
        lax.psum_scatter(partials[2], "tp", scatter_dimension=1, tiled=True).astype(jnp.float32),
        lax.psum_scatter(partials[3], "tp", scatter_dimension=1, tiled=True).astype(jnp.float32),
    )
    hidden, shared_hidden = (
        lax.all_gather(
            (jax.nn.silu(gate_part) * up_part).astype(jnp.bfloat16), "tp", axis=1, tiled=True
        ),
        lax.all_gather(
            (jax.nn.silu(sgate_part) * sup_part).astype(jnp.bfloat16), "tp", axis=1, tiled=True
        ),
    )
    produced = jnp.dot(hidden, down_new[0], preferred_element_type=jnp.float32).astype(jnp.bfloat16)
    returned = lax.all_to_all(
        produced.reshape(experts, capacity, portion_width),
        "fs",
        split_axis=0,
        concat_axis=0,
        tiled=True,
    )
    picked = returned.reshape(experts * capacity, portion_width)[target]
    routed = jnp.sum(routing_weight[:, :, None] * picked.astype(jnp.float32), axis=1)
    shared_out = jnp.dot(shared_hidden, shared_d, preferred_element_type=jnp.float32)
    mixed = (routed + shared_out).astype(jnp.bfloat16)
    return (mixed, gate_refreshed, up_new, down_new, shared_g, shared_u, shared_d)


MESH = pl.DeviceIdType.MESH


def nearest_first(n):
    orders = [sorted(range(n), key=lambda s: (abs(s - f), s)) for f in range(n)]
    return [sum(orders[f][i] * n**f for f in range(n)) for i in range(n)]


def fused_kernel(
    n_fs, n_tp, top_count,
    tok_ref, routes_ref, weight_ref, gain_ref, eg_ref, eu_ref, ed_ref, sg_ref, su_ref, sd_ref,
    mixed_ref, wout_ref,
    wall, tokbuf, meta_ref, metabuf, ssown, ssbuf, scown, scbuf, mt, sct, part, rsbuf, hid, outf, outb, retbuf,
    tok_s, tok_r, meta_s, meta_r, ss_s, ss_r, sc_s, sc_r, rs_s, rs_r, ag_s, ag_r,
    ret_s, ret_r, we_s, we_r, ws_s, ws_r, ye_s, ye_r, ys_s, ys_r,
):
    g, f, t = lax.axis_index("grp"), lax.axis_index("fs"), lax.axis_index("tp")
    rows, width = tok_ref.shape
    experts, units = eg_ref.shape[0], eg_ref.shape[1]
    sub = rows // n_tp
    half = units // 2
    f32, bf16 = jnp.float32, jnp.bfloat16
    code = nearest_first(n_fs)

    def source(i):
        total = 0
        digits = code[i]
        picks = [(digits // n_fs**q) % n_fs for q in range(n_fs)]
        for q in range(n_fs):
            hit = 1 - jnp.minimum(1, jnp.abs(f - q))
            total = total + picks[q] * hit
        return total

    def at_fs(index):
        return (g, index, t)

    def at_tp(index):
        return (g, f, index)

    partner = (1 - g, f, t)

    def remote(src, dst, send, recv, device):
        return pltpu.make_async_remote_copy(
            src_ref=src, dst_ref=dst, send_sem=send, recv_sem=recv,
            device_id=device, device_id_type=MESH,
        )

    fs_others = [lax.rem(f + j, n_fs) for j in range(1, n_fs)]
    tp_others = [lax.rem(t + j, n_tp) for j in range(1, n_tp)]

    barrier = pltpu.get_barrier_semaphore()
    peers = [at_fs(d) for d in fs_others] + [at_tp(d) for d in tp_others] + [partner]
    for device in peers:
        pl.semaphore_signal(barrier, inc=1, device_id=device, device_id_type=MESH)
    pl.semaphore_wait(barrier, len(peers))

    def to_right(src, dst, send, recv):
        @pl.when(f < n_fs - 1)
        def _():
            remote(src, dst, send, recv, at_fs(f + 1)).start()

    def to_left(src, dst, send, recv):
        @pl.when(f > 0)
        def _():
            remote(src, dst, send, recv, at_fs(f - 1)).start()

    def onward(s, ref, send, recv):
        @pl.when((s < f) & (f < n_fs - 1))
        def _():
            remote(ref, ref, send.at[s, 0], recv.at[s], at_fs(f + 1)).start()

        @pl.when((s > f) & (f > 0))
        def _():
            remote(ref, ref, send.at[s, 1], recv.at[s], at_fs(f - 1)).start()

    def line_sends_done(refs, send, recv):
        for s in range(n_fs):
            ref = refs(s)

            @pl.when((f >= s) & (f < n_fs - 1))
            def _():
                remote(ref, ref, send.at[s, 0], recv.at[s], at_fs(f + 1)).wait_send()

            @pl.when((f <= s) & (f > 0))
            def _():
                remote(ref, ref, send.at[s, 1], recv.at[s], at_fs(f - 1)).wait_send()

    meta_ref[...] = jnp.zeros(meta_ref.shape, f32)
    meta_ref[0:top_count, 0:rows] = routes_ref[...].astype(f32)
    meta_ref[top_count : 2 * top_count, 0:rows] = weight_ref[...]
    for go, way in ((to_right, 0), (to_left, 1)):
        go(meta_ref, metabuf.at[f], meta_s.at[f, way], meta_r.at[f])
        go(tok_ref, tokbuf.at[f], tok_s.at[f, way], tok_r.at[f])

    x = tok_ref[...].astype(f32)
    sq = x * x
    high = sq.astype(bf16)
    low = (sq - high.astype(f32)).astype(bf16)
    ones = jnp.ones((8, width), bf16)
    ssown[...] = jnp.zeros(ssown.shape, f32)
    ssown[:, 0:rows] = dense_rows(ones, high) + dense_rows(ones, low)
    for d in tp_others:
        remote(ssown, ssbuf.at[t], ss_s.at[d], ss_r.at[t], at_tp(d)).start()

    gain = gain_ref[...]
    for e in range(experts):
        wall[0, e] = (eg_ref[e] * gain).astype(bf16)
        wall[1, e] = (eu_ref[e] * gain).astype(bf16)
    wall[0, experts] = (sg_ref[...] * gain).astype(bf16)
    wall[1, experts] = (su_ref[...] * gain).astype(bf16)

    def transposed(row_ref):
        return jnp.transpose(row_ref[...])[0:rows]

    def forward_block(i, tokens, meta):
        mt[i] = transposed(meta)
        names = [mt[i, :, k : k + 1] for k in range(top_count)]
        columns = []
        for m in range(2):
            weight = wall[m].reshape((experts + 1) * units, width)
            sums = dense_rows(tokens[...], weight)
            for name in names:
                chosen = jnp.zeros((rows, units), f32)
                for e in range(experts):
                    chosen = jnp.where(name == float(e), sums[:, e * units : (e + 1) * units], chosen)
                columns.append(chosen)
            columns.append(sums[:, experts * units :])
        for c, column in enumerate(columns):
            part[i, :, :, c * units : (c + 1) * units] = column.astype(bf16).reshape(n_tp, sub, units)
        for d in tp_others:
            remote(part.at[i, d], rsbuf.at[i, t], rs_s.at[i, d], rs_r.at[i, t], at_tp(d)).start()

    def hidden_block(i, scale_row):
        sct[i] = transposed(scale_row)
        own_rows = pl.ds(pl.multiple_of(t * sub, 8), sub)
        scale = sct[i, own_rows, 0:1]
        weights = mt[i, own_rows, :]
        for d in tp_others:
            remote(part.at[i, d], rsbuf.at[i, d], rs_s.at[i, d], rs_r.at[i, d], at_tp(d)).wait_recv()
        total = part[i, t].astype(f32)
        for d in tp_others:
            total = total + rsbuf[i, d].astype(f32)
        total = total * scale
        kinds = top_count + 1
        for k in range(kinds):
            gate = total[:, k * units : (k + 1) * units]
            up = total[:, (kinds + k) * units : (kinds + k + 1) * units]
            value = jax.nn.silu(gate) * up
            if k < top_count:
                value = value * weights[:, top_count + k : top_count + k + 1]
            hid[i, t, :, k * units : (k + 1) * units] = value.astype(bf16)
        for d in tp_others:
            remote(hid.at[i, t], hid.at[i, t], ag_s.at[i, d], ag_r.at[i, t], at_tp(d)).start()

    def down_block(i):
        for d in tp_others:
            remote(hid.at[i, d], hid.at[i, d], ag_s.at[i, d], ag_r.at[i, d], at_tp(d)).wait_recv()
        values = hid[i].astype(f32).reshape(rows, (top_count + 1) * units)
        names = [mt[i, :, k : k + 1] for k in range(top_count)]
        spread = []
        for e in range(experts):
            chosen = jnp.zeros((rows, units), f32)
            for k, name in enumerate(names):
                chosen = jnp.where(name == float(e), values[:, k * units : (k + 1) * units], chosen)
            spread.append(chosen.astype(bf16))
        spread.append(values[:, top_count * units :].astype(bf16))
        weight = wall[2].reshape((experts + 1) * units, width)
        return jnp.dot(jnp.concatenate(spread, axis=1), weight, preferred_element_type=f32)

    def finish_block(i):
        product = down_block(i)
        if i == 0:
            outf[...] = product
        else:
            s = source(i)
            outb[i] = product.astype(bf16)
            remote(outb.at[i], retbuf.at[f], ret_s.at[i], ret_r.at[f], at_fs(s)).start()

    def token_block(i):
        s = source(i)
        remote(metabuf.at[s], metabuf.at[s], meta_s.at[s, 0], meta_r.at[s], partner).wait_recv()
        onward(s, metabuf.at[s], meta_s, meta_r)
        remote(tokbuf.at[s], tokbuf.at[s], tok_s.at[s, 0], tok_r.at[s], partner).wait_recv()
        onward(s, tokbuf.at[s], tok_s, tok_r)

    def scale_block(i):
        s = source(i)
        remote(scown, scbuf.at[s], sc_s.at[s], sc_r.at[s], partner).wait_recv()
        return scbuf.at[s]

    for e in range(experts):
        wall[2, e] = ed_ref[e].astype(bf16)
    wall[2, experts] = sd_ref[...].astype(bf16)

    mine = pl.ds(pl.multiple_of(g * half, 16), half)
    for way, go in ((0, to_right), (1, to_left)):
        go(wall.at[:, experts, mine], wout_ref.at[1, :, f, g], ws_s.at[f, way], ws_r.at[f])

    def give_expert(i):
        d = source(i)
        remote(
            wall.at[:, d, mine], wout_ref.at[0, :, f, g], we_s.at[d], we_r.at[f], at_fs(d)
        ).start()

    def pass_shared(i):
        s = source(i)
        shared = wout_ref.at[1, :, s, g]
        remote(shared, shared, ws_s.at[s, 0], ws_r.at[s], partner).wait_recv()
        onward(s, shared, ws_s, ws_r)
        remote(shared, shared, ys_s.at[s], ys_r.at[s], partner).start()

    def pass_routed(i):
        s = source(i)
        routed = wout_ref.at[0, :, s, g]
        remote(routed, routed, we_s.at[s], we_r.at[s], partner).wait_recv()
        remote(routed, routed, ye_s.at[s], ye_r.at[s], partner).start()

    forward_block(0, tok_ref, meta_ref)
    squares = ssown[...]
    for d in tp_others:
        remote(ssown, ssbuf.at[d], ss_s.at[d], ss_r.at[d], at_tp(d)).wait_recv()
        squares = squares + ssbuf[d]
    scown[...] = lax.rsqrt(squares / (width * n_tp) + norm_eps)
    for d in fs_others:
        remote(scown, scbuf.at[f], sc_s.at[d], sc_r.at[f], at_fs(d)).start()
    for h in range(2):
        wout_ref[0, :, f, h] = wall[:, f, h * half : (h + 1) * half]
        wout_ref[1, :, f, h] = wall[:, experts, h * half : (h + 1) * half]

    for i in range(1, n_fs):
        token_block(i)
        give_expert(n_fs - i)
        forward_block(i, tokbuf.at[source(i)], metabuf.at[source(i)])
        hidden_block(i - 1, scown if i == 1 else scale_block(i - 1))
        if i >= 2:
            finish_block(i - 2)
            pass_shared(i - 1)
    pass_routed(n_fs - 1)
    hidden_block(n_fs - 1, scale_block(n_fs - 1))
    finish_block(n_fs - 2)
    finish_block(n_fs - 1)
    pass_shared(n_fs - 1)
    for i in range(n_fs - 2, 0, -1):
        pass_routed(i)

    total = outf[...]
    for d in fs_others:
        remote(retbuf.at[d], retbuf.at[d], ret_s.at[1], ret_r.at[d], partner).wait_recv()
        total = total + retbuf[d].astype(f32)
    mixed_ref[...] = total.astype(bf16)

    for d in fs_others:
        shared, routed = wout_ref.at[1, :, d, 1 - g], wout_ref.at[0, :, d, 1 - g]
        remote(shared, shared, ys_s.at[d], ys_r.at[d], partner).wait_recv()
        remote(routed, routed, ye_s.at[d], ye_r.at[d], partner).wait_recv()

    line_sends_done(lambda s: metabuf.at[s], meta_s, meta_r)
    line_sends_done(lambda s: tokbuf.at[s], tok_s, tok_r)
    line_sends_done(lambda s: wout_ref.at[1, :, s, g], ws_s, ws_r)
    for d in tp_others:
        remote(ssown, ssbuf.at[t], ss_s.at[d], ss_r.at[t], at_tp(d)).wait_send()
        for i in range(n_fs):
            remote(part.at[i, d], rsbuf.at[i, t], rs_s.at[i, d], rs_r.at[i, t], at_tp(d)).wait_send()
            remote(hid.at[i, t], hid.at[i, t], ag_s.at[i, d], ag_r.at[i, t], at_tp(d)).wait_send()
    for j, d in enumerate(fs_others):
        remote(scown, scbuf.at[f], sc_s.at[d], sc_r.at[f], at_fs(d)).wait_send()
        remote(outb.at[j + 1], retbuf.at[f], ret_s.at[j + 1], ret_r.at[f], at_fs(d)).wait_send()
        shared, routed = wout_ref.at[1, :, d, g], wout_ref.at[0, :, d, g]
        remote(routed, routed, we_s.at[d], we_r.at[f], at_fs(d)).wait_send()
        remote(shared, shared, ys_s.at[d], ys_r.at[d], partner).wait_send()
        remote(routed, routed, ye_s.at[d], ye_r.at[d], partner).wait_send()


def per_device_fused(
    tokens,
    routes,
    routing_weight,
    norm_gain_vector,
    expert_gate,
    expert_up,
    expert_down,
    shared_gate,
    shared_up,
    shared_down,
):
    n_fs, n_tp = lax.axis_size("fs"), lax.axis_size("tp")
    rows, width = tokens.shape
    experts, units, _ = expert_gate.shape
    top_count = routes.shape[1]
    sub, half = rows // n_tp, units // 2
    meta_rows = -(-2 * top_count // 8) * 8
    lanes = -(-rows // 128) * 128
    f32, bf16 = jnp.float32, jnp.bfloat16
    kinds = top_count + 1
    dma = pltpu.SemaphoreType.DMA
    vmem = pl.BlockSpec(memory_space=pltpu.VMEM)
    mixed, served = pl.pallas_call(
        functools.partial(fused_kernel, n_fs, n_tp, top_count),
        out_shape=(
            jax.ShapeDtypeStruct((rows, width), bf16),
            jax.ShapeDtypeStruct((2, 3, n_fs, 2, half, width), bf16),
        ),
        in_specs=[vmem] * 10,
        out_specs=(vmem, vmem),
        scratch_shapes=[
            pltpu.VMEM((3, experts + 1, units, width), bf16),
            pltpu.VMEM((n_fs, rows, width), bf16),
            pltpu.VMEM((meta_rows, lanes), f32),
            pltpu.VMEM((n_fs, meta_rows, lanes), f32),
            pltpu.VMEM((8, lanes), f32),
            pltpu.VMEM((n_tp, 8, lanes), f32),
            pltpu.VMEM((8, lanes), f32),
            pltpu.VMEM((n_fs, 8, lanes), f32),
            pltpu.VMEM((n_fs, rows, meta_rows), f32),
            pltpu.VMEM((n_fs, rows, 8), f32),
            pltpu.VMEM((n_fs, n_tp, sub, 2 * kinds * units), bf16),
            pltpu.VMEM((n_fs, n_tp, sub, 2 * kinds * units), bf16),
            pltpu.VMEM((n_fs, n_tp, sub, kinds * units), bf16),
            pltpu.VMEM((rows, width), f32),
            pltpu.VMEM((n_fs, rows, width), bf16),
            pltpu.VMEM((n_fs, rows, width), bf16),
            dma((n_fs, 2)), dma((n_fs,)),
            dma((n_fs, 2)), dma((n_fs,)),
            dma((n_tp,)), dma((n_tp,)),
            dma((n_fs,)), dma((n_fs,)),
            dma((n_fs, n_tp)), dma((n_fs, n_tp)),
            dma((n_fs, n_tp)), dma((n_fs, n_tp)),
            dma((n_fs,)), dma((n_fs,)),
            dma((n_fs,)), dma((n_fs,)),
            dma((n_fs, 2)), dma((n_fs,)),
            dma((n_fs,)), dma((n_fs,)),
            dma((n_fs,)), dma((n_fs,)),
        ],
        compiler_params=pltpu.CompilerParams(
            collective_id=0, has_side_effects=True, vmem_limit_bytes=60 * 1024 * 1024
        ),
        name="hand_over_and_layer",
    )(
        tokens, routes.T, routing_weight.T, norm_gain_vector[None, :],
        expert_gate, expert_up, expert_down, shared_gate, shared_up, shared_down,
    )
    served = served.reshape(2, 3, n_fs * units, width)
    return (
        mixed,
        served[0, 0][None], served[0, 1][None], served[0, 2][None],
        served[1, 0], served[1, 1], served[1, 2],
    )


def per_device(tokens, routes, routing_weight, norm_gain_vector, *weights):
    experts, units, width = weights[0].shape
    rows, n_fs, n_tp = tokens.shape[0], lax.axis_size("fs"), lax.axis_size("tp")
    whole_tiles = units % 128 == 0 and width % 128 == 0 and rows % (16 * n_tp) == 0
    fits = (experts + 1) * units * width <= 2**20 and n_fs <= 4 and n_tp <= 4
    chosen = per_device_plain
    if whole_tiles and fits and experts == n_fs and lax.axis_size("grp") == 2 and n_fs > 2:
        chosen = per_device_fused
    return chosen(tokens, routes, routing_weight, norm_gain_vector, *weights)


def solution(mesh):
    return jax.shard_map(
        per_device,
        mesh=mesh,
        in_specs=(
            P(("grp", "fs"), "tp"),
            P(("grp", "fs"), None),
            P(("grp", "fs"), None),
            P("tp"),
            P(None, "fs", "tp"),
            P(None, "fs", "tp"),
            P(None, "fs", "tp"),
            P("fs", "tp"),
            P("fs", "tp"),
            P("fs", "tp"),
        ),
        out_specs=(
            P(("grp", "fs"), "tp"),
            P(("grp", "fs"), None, "tp"),
            P(("grp", "fs"), None, "tp"),
            P(("grp", "fs"), None, "tp"),
            P("grp", "tp"),
            P("grp", "tp"),
            P("grp", "tp"),
        ),
        check_vma=False,
    )
```
